32 devices in a mesh: sp: 16 (over z, y, x), tp: 2 (over core).
Axes of the slice: x: 2, y: 2, z: 4, core: 2. Of those that a mesh axis runs over, the one named last changes fastest.
Arguments:
- stream_signals: bfloat16 [2048, 1024], P('sp', 'tp'), may hold values from -6 to 6
- cluster_entry_matrices: bfloat16 [2048, 256], P('sp', 'tp'), may hold values from -6 to 6
- cluster_exit_matrices: bfloat16 [2048, 256], P('sp', 'tp'), may hold values from -6 to 6
- valve_logits: bfloat16 [2048, 1024], P('sp', 'tp'), may hold values from -12 to 12
- stride_logits: bfloat16 [2048, 16], P('sp', 'tp'), may hold values from -2.7 to 2.7
- surplus_log_fading: float32 [2048, 16], P('sp', 'tp'), may hold values from -0.69 to 0
- stream_filter_coefficients: bfloat16 [4, 1024], P(None, 'tp'), may hold values from -3 to 3
- entry_filter_coefficients: bfloat16 [4, 256], P(None, 'tp'), may hold values from -3 to 3
- exit_filter_coefficients: bfloat16 [4, 256], P(None, 'tp'), may hold values from -3 to 3
- stride_offset_vector: float32 [16], P('tp'), may hold values from -3.3 to 1.3
- channel_fading_speed: float32 [16], P('tp'), may hold values from 0 to 0.03
- rescale_amplitude: bfloat16 [1024], P('tp'), may hold values from 0.099609375 to 1.8984375
- final_linear_matrix: bfloat16 [1024, 2048], P('tp'), may hold values from -0.1875 to 0.1875
Outputs:
- merged: bfloat16 [2048, 2048], P(('sp', 'tp'))
The draws below stay inside these ranges and needn't reach their ends.
All inputs are finite; a program needn't handle non-finite values.
Results may differ from the reference program's by a relative error of at most 0.013.
Values may be sent and summed in bfloat16 or wider, within the bound.
A program may use at most 128 MiB of HBM per device.

```python
import math
import jax
import jax.numpy as jnp
from jax import lax

D = 2048
HEADS = 16
HEAD_DIM = 64
GROUPS = 4
STATE = 64
CONV = 4
SPAN = 128
SEQ = 2048
INNER = 1024
GW = 256
N_TP = 2


def draw_valve_logits(key, part):
    scales = jnp.exp(jnp.linspace(math.log(0.5), math.log(3.0), INNER))
    basis = jnp.clip(jax.random.normal(key, (SEQ, INNER), jnp.float32), -4.0, 4.0)
    return (basis * scales[None]).astype(jnp.bfloat16)


def draw_stride_logits(key, part):
    jitter_key = jax.random.fold_in(key, 31)
    shift_key = jax.random.fold_in(key, 32)
    blocks = SEQ // SPAN
    jitter = jnp.clip(0.5 * jax.random.normal(jitter_key, (SEQ, HEADS), jnp.float32), -2.0, 2.0)
    offset = jax.random.uniform(shift_key, (blocks, 1, HEADS), jnp.float32, -0.7, 0.7)
    return (jitter.reshape(blocks, SPAN, HEADS) + offset).reshape(SEQ, HEADS).astype(jnp.bfloat16)


def slow_heads(key):
    ordering = jax.random.permutation(jax.random.fold_in(key, 11), HEADS)
    kept = HEADS // 2
    return ordering < kept


def draw_stride_offset_vector(key, part):
    slow = slow_heads(key)
    jitter = jax.random.uniform(jax.random.fold_in(key, 12), (HEADS,), jnp.float32, -0.3, 0.3)
    return jnp.where(slow, -3.0 + jitter, 1.0 + jitter)


def draw_channel_fading_speed(key, part):
    slow = slow_heads(key)
    level = jax.random.uniform(jax.random.fold_in(key, 13), (HEADS,), jnp.float32, 0.0, 1.0)
    slow_rate = jnp.exp(math.log(0.1) + level * math.log(8.0)) / (SEQ * 0.06)
    fast_rate = jnp.exp(math.log(0.012) + level * math.log(2.5))
    return jnp.where(slow, slow_rate, fast_rate)


def draw_surplus_log_fading(key, part):
    places = jax.random.randint(jax.random.fold_in(key, 21), (3,), 0, SEQ)
    depths = jax.random.uniform(jax.random.fold_in(key, 22), (3, HEADS), jnp.float32, 0.22, 0.69)
    row_ids = lax.iota(jnp.int32, SEQ)
    struck = (row_ids[:, None] == places[None, :]).astype(jnp.float32)
    return -jnp.minimum(jnp.dot(struck, depths, precision=lax.Precision.HIGHEST), 0.69)


def block_scale(rng, dims, cuts, smallest, largest):
    loudness, own = 1.0, jax.random.fold_in(rng, 6)
    for dim, shards_of in cuts:
        heights = jnp.exp(jax.random.uniform(jax.random.fold_in(own, dim), (shards_of,), jnp.float32, smallest / len(cuts), largest / len(cuts)))
        loudness = loudness * jnp.repeat(heights, dims[dim] // shards_of).reshape([-1 if axis == dim else 1 for axis in range(len(dims))])
    return loudness


def centred(own_key, dims, scale, bound, shards=(), held_as=jnp.bfloat16):
    entries = jax.random.normal(own_key, dims, jnp.float32) * scale
    if len(shards) > 0:
        entries = block_scale(own_key, dims, shards, -0.22, 0.18) * entries
    return jnp.clip(entries, min=-bound, max=bound).astype(held_as)


def setup_inputs(seed: int = 0) -> dict:
    splits = jax.random.split(jax.random.key(seed), 14)
    stream_signals = centred(splits[0], (SEQ, INNER), 1.0, 6.0, ((0, 16), (1, 2)))
    cluster_entry_matrices = centred(splits[1], (SEQ, GW), 1.0, 6.0, ((0, 16), (1, 2)))
    cluster_exit_matrices = centred(splits[2], (SEQ, GW), 1.0, 6.0, ((0, 16), (1, 2)))
    valve_logits = draw_valve_logits(jax.random.fold_in(splits[13], 71), 0)
    stride_logits = draw_stride_logits(jax.random.fold_in(splits[13], 71), 0)
    surplus_log_fading = draw_surplus_log_fading(jax.random.fold_in(splits[13], 71), 0)
    stream_filter_coefficients = centred(splits[6], (CONV, INNER), CONV ** -0.5, 3.0, ((1, 2),))
    entry_filter_coefficients = centred(splits[7], (CONV, GW), CONV ** -0.5, 3.0, ((1, 2),))
    exit_filter_coefficients = centred(splits[8], (CONV, GW), CONV ** -0.5, 3.0, ((1, 2),))
    stride_offset_vector = draw_stride_offset_vector(jax.random.fold_in(splits[13], 71), 0)
    channel_fading_speed = draw_channel_fading_speed(jax.random.fold_in(splits[13], 71), 0)
    rescale_amplitude = jnp.clip(1.0 + 0.18 * jax.random.normal(splits[11], (INNER,), jnp.float32), 0.099609375, 1.8984375).astype(jnp.bfloat16)
    final_linear_matrix = centred(splits[12], (INNER, D), INNER ** -0.5, 0.1875, ((0, 2),))
    return {"stream_signals": stream_signals, "cluster_entry_matrices": cluster_entry_matrices, "cluster_exit_matrices": cluster_exit_matrices, "valve_logits": valve_logits, "stride_logits": stride_logits, "surplus_log_fading": surplus_log_fading, "stream_filter_coefficients": stream_filter_coefficients, "entry_filter_coefficients": entry_filter_coefficients, "exit_filter_coefficients": exit_filter_coefficients, "stride_offset_vector": stride_offset_vector, "channel_fading_speed": channel_fading_speed, "rescale_amplitude": rescale_amplitude, "final_linear_matrix": final_linear_matrix}


EPS = 1e-05
FULL_PRECISION = lax.Precision.HIGHEST

def conv_silu(signal, prior, kernel):
    length = signal.shape[0]
    joined = jnp.concatenate([prior, signal], axis=0).astype(jnp.float32)
    taps = kernel.astype(jnp.float32)
    summed = jnp.zeros(signal.shape, jnp.float32)
    for offset in range(kernel.shape[0]):
        summed = summed + taps[offset] * joined[offset:offset + length]
    return jax.nn.silu(summed).astype(jnp.bfloat16)

def block_terms(conv_x, conv_b, conv_c, stride_length, within_segment):
    length = conv_x.shape[0]
    groups = conv_b.shape[1] // STATE
    head_count = stride_length.shape[1]
    per_group = head_count // groups
    b_heads = conv_b.reshape(length, groups, STATE).astype(jnp.float32)
    c_heads = conv_c.reshape(length, groups, STATE).astype(jnp.float32)
    x_scaled = (conv_x.astype(jnp.float32).reshape(length, head_count, HEAD_DIM) * stride_length[:, :, None]).astype(jnp.bfloat16)
    scores = jnp.einsum('tgn,sgn->gts', c_heads, b_heads, precision=FULL_PRECISION)
    gap_log = within_segment.T[:, :, None] - within_segment.T[:, None, :]
    causal = lax.iota(jnp.int32, length)[:, None] >= lax.iota(jnp.int32, length)[None, :]
    decays = jnp.exp(jnp.where(causal[None], gap_log, -jnp.inf)).reshape(groups, per_group, length, length)
    decay_weights = (scores[:, None] * decays).astype(jnp.bfloat16)
    head_input_rows = x_scaled.reshape(length, groups, per_group, HEAD_DIM).astype(jnp.float32)
    intra_block_term = jnp.einsum('wbzv,vwbi->zwbi', decay_weights.astype(jnp.float32), head_input_rows, precision=FULL_PRECISION)
    block_decay = within_segment[-1]
    to_end = jnp.exp(block_decay[None] - within_segment).reshape(length, groups, per_group)
    b_end = (to_end[..., None] * b_heads[:, :, None, :]).astype(jnp.bfloat16)
    block_state = jnp.einsum('sgrp,sgrn->grpn', head_input_rows, b_end.astype(jnp.float32), precision=FULL_PRECISION)
    growth = jnp.exp(within_segment).reshape(length, groups, per_group)
    return (intra_block_term, block_state, block_decay.reshape(groups, per_group), c_heads, growth)

def read_state(c_heads, growth, entering):
    return growth[..., None] * jnp.einsum('tgn,grpn->tgrp', c_heads, entering, precision=FULL_PRECISION)

def reference(stream_signals, cluster_entry_matrices, cluster_exit_matrices, valve_logits, stride_logits, surplus_log_fading, stream_filter_coefficients, entry_filter_coefficients, exit_filter_coefficients, stride_offset_vector, channel_fading_speed, rescale_amplitude, final_linear_matrix):
    conv_x = conv_silu(stream_signals, jnp.zeros((CONV - 1, INNER), jnp.bfloat16), stream_filter_coefficients)
    conv_b = conv_silu(cluster_entry_matrices, jnp.zeros((CONV - 1, GW), jnp.bfloat16), entry_filter_coefficients)
    conv_c = conv_silu(cluster_exit_matrices, jnp.zeros((CONV - 1, GW), jnp.bfloat16), exit_filter_coefficients)
    stride_length = jax.nn.softplus(stride_logits.astype(jnp.float32) + stride_offset_vector[None])
    stride_log_values = surplus_log_fading - stride_length * channel_fading_speed[None]
    blocks = SEQ // SPAN
    per_group = HEADS // GROUPS

    def advance(carried, pieces):
        block_x, block_b, block_c, block_step, block_logs = pieces
        within_segment = jnp.cumsum(block_logs, axis=0)
        intra_block_term, block_state, block_decay, c_heads, growth = block_terms(block_x, block_b, block_c, block_step, within_segment)
        values = intra_block_term + read_state(c_heads, growth, carried)
        updated = jnp.exp(block_decay)[:, :, None, None] * carried + block_state
        return (updated, values.reshape(SPAN, INNER))
    stacked = (conv_x.reshape(blocks, SPAN, INNER), conv_b.reshape(blocks, SPAN, GW), conv_c.reshape(blocks, SPAN, GW), stride_length.reshape(blocks, SPAN, HEADS), stride_log_values.reshape(blocks, SPAN, HEADS))
    start = jnp.zeros((GROUPS, per_group, HEAD_DIM, STATE), jnp.float32)
    _, outputs = lax.scan(advance, start, stacked)
    gated = outputs.reshape(SEQ, INNER) * jax.nn.silu(valve_logits.astype(jnp.float32))
    scale = lax.rsqrt(lax.optimization_barrier(jnp.mean(gated * gated, axis=1)) + EPS)
    normed = (gated * scale[:, None] * rescale_amplitude.astype(jnp.float32)[None]).astype(jnp.bfloat16)
    part_width = INNER // N_TP
    summed = jnp.zeros((SEQ, D), jnp.float32)
    for member in range(N_TP):
        portion = jnp.dot(normed[:, member * part_width:(member + 1) * part_width], final_linear_matrix[member * part_width:(member + 1) * part_width], preferred_element_type=jnp.float32).astype(jnp.bfloat16)
        summed = summed + lax.optimization_barrier(portion).astype(jnp.float32)
    return summed.astype(jnp.bfloat16)
```

```python
import functools

import jax
import jax.numpy as jnp
from jax import lax
from jax.experimental import pallas as pl
from jax.experimental.pallas import tpu as pltpu
from jax.sharding import PartitionSpec as P

HEAD_DIM = 64
STATE = 64
LANES = 128
EPS = 1e-05
EXACT = lax.Precision.HIGHEST
MESH = pl.DeviceIdType.MESH
F32 = jnp.float32
BF16 = jnp.bfloat16


def silu(v):
    return v / (1.0 + jnp.exp(-v))


def kernel(
    n, owners,
    x_ref, b_ref, c_ref, z_hbm, dt_ref, fade_ref, tx_ref, tb_ref, tc_ref,
    off_ref, speed_ref, gain_ref, w_hbm,
    out_ref,
    z_ref, w_ref, halo_x, halo_b, halo_c, joined, xs, xe, cb, cc, step_e, end_e, grow_e,
    gate, y_in, dec, dec_in, st, st_in, eb, ent, gg, ssq, ssq_in, p_out, p_in,
    loc_sem, hs, hr, ds_, dr, s1, r1, s2, r2, sx, rx,
):
    length, inner = x_ref.shape
    gw = b_ref.shape[1]
    heads = dt_ref.shape[0]
    tiles = inner // LANES
    per_group_tiles = tiles // (gw // STATE)
    stride = n // owners
    rows = tiles * STATE // owners
    taps = tx_ref.shape[0]
    half = length // 2
    chunks, _, cols = p_out.shape
    me = lax.axis_index("sp")
    core = lax.axis_index("tp")
    mate = 1 - core

    z_copy = pltpu.make_async_copy(z_hbm, z_ref, loc_sem.at[0])
    w_copy = pltpu.make_async_copy(w_hbm, w_ref, loc_sem.at[1])
    z_copy.start()
    w_copy.start()

    barrier = pltpu.get_barrier_semaphore()

    def greet(i, carry):
        pl.semaphore_signal(
            barrier, inc=1, device_id={"sp": lax.rem(me + i, n)}, device_id_type=MESH
        )
        return carry

    lax.fori_loop(1, n, greet, 0)
    pl.semaphore_signal(barrier, inc=1, device_id={"tp": mate}, device_id_type=MESH)

    sub = lax.broadcasted_iota(jnp.int32, (heads, length), 0)
    off = jnp.zeros((heads, length), F32)
    speed = jnp.zeros((heads, length), F32)
    for h in range(heads):
        off = jnp.where(sub == h, off_ref[h], off)
        speed = jnp.where(sub == h, speed_ref[h], speed)
    v = dt_ref[...].astype(F32) + off
    step_t = jnp.maximum(v, 0.0) + jnp.log1p(jnp.exp(-jnp.abs(v)))
    log_t = fade_ref[...] - step_t * speed
    r_i = lax.broadcasted_iota(jnp.int32, (length, length), 0)
    c_i = lax.broadcasted_iota(jnp.int32, (length, length), 1)
    causal = r_i >= c_i
    lower = causal.astype(F32)
    eye = (r_i == c_i).astype(F32)
    nt = (((1,), (1,)), ((), ()))
    within = lax.dot_general(lower, log_t, nt, precision=EXACT, preferred_element_type=F32)
    step = lax.dot_general(eye, step_t, nt, precision=EXACT, preferred_element_type=F32)
    within_t = lax.dot_general(log_t, lower, nt, precision=EXACT, preferred_element_type=F32)
    spread = (
        lax.broadcasted_iota(jnp.int32, (heads, inner), 0)
        == lax.broadcasted_iota(jnp.int32, (heads, inner), 1) // HEAD_DIM
    ).astype(F32)
    step_e[...] = jnp.dot(step, spread, precision=EXACT, preferred_element_type=F32)
    within_e = jnp.dot(within, spread, precision=EXACT, preferred_element_type=F32)
    last = within_e[length - 1 :]
    end_e[...] = jnp.exp(last - within_e)
    grow_e[...] = jnp.exp(within_e)
    whole = jnp.exp(last)
    for t in range(tiles):
        dec[t] = whole[:, t * LANES : (t + 1) * LANES]

    lead = 8
    joined[:lead] = jnp.zeros((lead, inner + 2 * gw), F32)
    joined[lead:, :inner] = x_ref[...].astype(F32)
    joined[lead:, inner : inner + gw] = b_ref[...].astype(F32)
    joined[lead:, inner + gw :] = c_ref[...].astype(F32)

    def conv(tap_ref, first, width, start, count):
        coef = tap_ref[...].astype(F32)
        total = jnp.zeros((count, width), F32)
        for k in range(taps):
            begin = lead - (taps - 1) + k + start
            total += coef[k : k + 1] * joined[begin : begin + count, first : first + width]
        return silu(total).astype(BF16)

    def mixed(start, count):
        where = slice(start, start + count)
        scaled = conv(tx_ref, 0, inner, start, count).astype(F32) * step_e[where]
        xs[where] = scaled.astype(BF16)
        xe[where] = (scaled * end_e[where]).astype(BF16)
        cb[where] = conv(tb_ref, inner, gw, start, count)
        cc[where] = conv(tc_ref, inner + gw, gw, start, count)

    mixed(0, length)

    pl.semaphore_wait(barrier, n)

    edge = halo_x.shape[0]
    halos = [
        pltpu.make_async_remote_copy(
            src_ref=src.at[pl.ds(length - edge, edge)],
            dst_ref=dst,
            send_sem=hs.at[i],
            recv_sem=hr.at[i],
            device_id={"sp": lax.rem(me + 1, n)},
            device_id_type=MESH,
        )
        for i, (src, dst) in enumerate(((x_ref, halo_x), (b_ref, halo_b), (c_ref, halo_c)))
    ]

    @pl.when(me < n - 1)
    def _():
        for copy in halos:
            copy.start()

    base = me // stride
    tile_of = owners // tiles

    def dec_copy(owner, slot):
        return pltpu.make_async_remote_copy(
            src_ref=dec.at[owner // tile_of],
            dst_ref=dec_in.at[slot],
            send_sem=ds_.at[owner],
            recv_sem=dr.at[slot],
            device_id={"sp": owner * stride},
            device_id_type=MESH,
        )

    def st_copy(owner, slot):
        return pltpu.make_async_remote_copy(
            src_ref=st.at[owner],
            dst_ref=st_in.at[slot],
            send_sem=s1.at[owner],
            recv_sem=r1.at[slot],
            device_id={"sp": owner * stride},
            device_id_type=MESH,
        )

    def ent_copy(place, slot):
        return pltpu.make_async_remote_copy(
            src_ref=eb.at[place],
            dst_ref=ent.at[slot],
            send_sem=s2.at[place],
            recv_sem=r2.at[slot],
            device_id={"sp": place},
            device_id_type=MESH,
        )

    def to_owners(make, method, slot):
        def body(i, carry):
            owner = lax.rem(base + i, owners)

            @pl.when(owner * stride != me)
            def _():
                getattr(make(owner, slot), method)()

            return carry

        lax.fori_loop(0, owners, body, 0)

    is_owner = lax.rem(me, stride) == 0
    to_owners(dec_copy, "start", me)

    @pl.when(is_owner)
    def _():
        dec_in[me] = dec[base // tile_of]

    @pl.when(me > 0)
    def _():
        for copy in halos:
            copy.wait_recv()
        joined[:lead, :inner] = halo_x[...].astype(F32)[edge - lead :]
        joined[:lead, inner : inner + gw] = halo_b[...].astype(F32)[edge - lead :]
        joined[:lead, inner + gw :] = halo_c[...].astype(F32)[edge - lead :]
        mixed(0, 16)

    cb_t = cb[...].astype(F32).T.astype(BF16)
    per_tile = STATE // rows
    for t in range(tiles):
        g = t // per_group_tiles
        s = jnp.dot(
            cb_t[g * STATE : (g + 1) * STATE],
            xe[:, t * LANES : (t + 1) * LANES],
            preferred_element_type=F32,
        )
        for j in range(per_tile):
            st[t * per_tile + j] = s[j * rows : (j + 1) * rows].astype(BF16)

    to_owners(st_copy, "start", me)

    @pl.when(is_owner)
    def _():
        st_in[me] = st[base]

    low_lanes = lax.broadcasted_iota(jnp.int32, (length, LANES), 1) < HEAD_DIM
    for t in range(tiles):
        g = t // per_group_tiles
        if t % per_group_tiles == 0:
            scores = jnp.dot(
                cc[:, g * STATE : (g + 1) * STATE],
                cb_t[g * STATE : (g + 1) * STATE],
                preferred_element_type=F32,
            )
        parts = []
        for h in (2 * t, 2 * t + 1):
            gap = within[:, h : h + 1] - within_t[h : h + 1]
            weight = (scores * jnp.exp(jnp.where(causal, gap, -jnp.inf))).astype(BF16)
            parts.append(
                jnp.dot(
                    weight, xs[:, t * LANES : (t + 1) * LANES], preferred_element_type=F32
                )
            )
        y_in[:, t * LANES : (t + 1) * LANES] = jnp.where(low_lanes, parts[0], parts[1])
    z_copy.wait()
    gate[...] = silu(z_ref[...].astype(F32))

    @pl.when(is_owner)
    def _():
        def turn(k, state):
            @pl.when(k != me)
            def _():
                dec_copy(base, k).wait_recv()
                st_copy(base, k).wait_recv()

            eb[k] = state.astype(BF16)
            return dec_in[k] * state + st_in[k].astype(F32)

        lax.fori_loop(0, n, turn, jnp.zeros((rows, LANES), F32))

        def deliver(i, carry):
            ent_copy(lax.rem(me + i, n), base).start()
            return carry

        lax.fori_loop(1, n, deliver, 0)
        ent[base] = eb[me]

    def arrive(owner, carry):
        @pl.when(owner * stride != me)
        def _():
            ent_copy(me, owner).wait_recv()

        return carry

    lax.fori_loop(0, owners, arrive, 0)

    total = jnp.zeros((length, 1), F32)
    for t in range(tiles):
        g = t // per_group_tiles
        lanes = slice(t * LANES, (t + 1) * LANES)
        held = ent[t * per_tile : (t + 1) * per_tile].reshape(STATE, LANES)
        read = jnp.dot(cc[:, g * STATE : (g + 1) * STATE], held, preferred_element_type=F32)
        gated = (y_in[:, lanes] + grow_e[:, lanes] * read) * gate[:, lanes]
        total += jnp.sum(gated * gated, axis=1, keepdims=True)
        gg[:, lanes] = (gated * gain_ref[:, lanes].astype(F32)).astype(BF16)
    ssq[...] = jnp.broadcast_to(total, (length, LANES))

    def mate_copy(src, dst, i):
        return pltpu.make_async_remote_copy(
            src_ref=src,
            dst_ref=dst,
            send_sem=sx.at[i],
            recv_sem=rx.at[i],
            device_id={"tp": mate},
            device_id_type=MESH,
        )

    theirs = pl.ds(pl.multiple_of(mate * half, half), half)
    mine = pl.ds(pl.multiple_of(core * half, half), half)
    w_copy.wait()
    sent = []
    for i in range(chunks):
        p_out[i] = jnp.dot(
            gg[theirs], w_ref[:, i * cols : (i + 1) * cols], preferred_element_type=F32
        ).astype(BF16)
        if i == 0:
            first = mate_copy(ssq.at[theirs], ssq_in, chunks)
            first.start()
        copy = mate_copy(p_out.at[i], p_in.at[i], i)
        copy.start()
        sent.append(copy)
    own = [
        jnp.dot(gg[mine], w_ref[:, i * cols : (i + 1) * cols], preferred_element_type=F32)
        for i in range(chunks)
    ]
    first.wait_recv()
    mean = (ssq[mine] + ssq_in[...]) * (1.0 / (2 * inner))
    scale = lax.rsqrt(mean + EPS)[:, :1]
    for i in range(chunks):
        sent[i].wait_recv()
        out_ref[:, i * cols : (i + 1) * cols] = (
            (own[i] + p_in[i].astype(F32)) * scale
        ).astype(BF16)

    @pl.when(me < n - 1)
    def _():
        for copy in halos:
            copy.wait_send()

    to_owners(dec_copy, "wait_send", me)
    to_owners(st_copy, "wait_send", me)

    @pl.when(is_owner)
    def _():
        def sent_one(i, carry):
            ent_copy(lax.rem(me + i, n), base).wait_send()
            return carry

        lax.fori_loop(1, n, sent_one, 0)

    first.wait_send()
    for copy in sent:
        copy.wait_send()


def per_device(n, x, b, c, z, dt, fade, tx, tb, tc, off, speed, gain, w):
    length, inner = x.shape
    gw = b.shape[1]
    width = w.shape[1]
    tiles = inner // LANES
    owners = min(n, tiles * STATE // 16)
    rows = tiles * STATE // owners
    half = length // 2
    chunks = 4
    cols = width // chunks
    vmem = pl.BlockSpec(memory_space=pltpu.VMEM)
    smem = pl.BlockSpec(memory_space=pltpu.SMEM)
    hbm = pl.BlockSpec(memory_space=pl.ANY)
    V = pltpu.VMEM
    dma = lambda k: pltpu.SemaphoreType.DMA((k,))
    return pl.pallas_call(
        functools.partial(kernel, n, owners),
        out_shape=jax.ShapeDtypeStruct((half, width), BF16),
        in_specs=[vmem, vmem, vmem, hbm, vmem, vmem, vmem, vmem, vmem, smem, smem, vmem, hbm],
        out_specs=vmem,
        scratch_shapes=[
            V((length, inner), BF16),
            V(w.shape, BF16),
            V((16, inner), BF16),
            V((16, gw), BF16),
            V((16, gw), BF16),
            V((length + 8, inner + 2 * gw), F32),
            V((length, inner), BF16),
            V((length, inner), BF16),
            V((length, gw), BF16),
            V((length, gw), BF16),
            V((length, inner), F32),
            V((length, inner), F32),
            V((length, inner), F32),
            V((length, inner), F32),
            V((length, inner), F32),
            V((tiles, 1, LANES), F32),
            V((n, 1, LANES), F32),
            V((owners, rows, LANES), BF16),
            V((n, rows, LANES), BF16),
            V((n, rows, LANES), BF16),
            V((owners, rows, LANES), BF16),
            V((length, inner), BF16),
            V((length, LANES), F32),
            V((half, LANES), F32),
            V((chunks, half, cols), BF16),
            V((chunks, half, cols), BF16),
            dma(2), dma(3), dma(3), dma(owners), dma(n), dma(owners), dma(n),
            dma(n), dma(owners), dma(chunks + 1), dma(chunks + 1),
        ],
        compiler_params=pltpu.CompilerParams(collective_id=0, has_side_effects=True),
    )(x, b, c, z, dt.T, fade.T, tx, tb, tc, off, speed, gain.reshape(1, inner), w)


def solution(mesh):
    both = P("sp", "tp")
    taps = P(None, "tp")
    placed = (both,) * 6 + (taps,) * 3 + (P("tp"),) * 3 + (P("tp", None),)
    return jax.shard_map(
        functools.partial(per_device, mesh.shape["sp"]),
        mesh=mesh,
        in_specs=placed,
        out_specs=P(("sp", "tp"), None),
        check_vma=False,
    )
```

```python
import functools

import jax
import jax.numpy as jnp
from jax import lax
from jax.experimental import pallas as pl
from jax.experimental.pallas import tpu as pltpu
from jax.sharding import PartitionSpec as P

HEAD_DIM = 64
STATE = 64
LANES = 128
EPS = 1e-05
EXACT = lax.Precision.HIGHEST
MESH = pl.DeviceIdType.MESH
F32 = jnp.float32
BF16 = jnp.bfloat16


def silu(v):
    return v / (1.0 + jnp.exp(-v))


def kernel(
    n, owners,
    x_hbm, b_hbm, c_hbm, z_hbm, dt_hbm, fade_hbm, tx_hbm, tb_hbm, tc_hbm,
    off_hbm, speed_hbm, gain_hbm, w_hbm,
    out_ref,
    x_ref, b_ref, c_ref, z_ref, dt_ref, fade_ref, tx_ref, tb_ref, tc_ref,
    off_ref, speed_ref, gain_ref, w_ref, halo_x, halo_b, halo_c, joined, xs, xe, cb, cc, step_e, end_e, grow_e,
    gate, y_in, dec, dec_in, st, st_in, eb, ent, gg, ssq, ssq_in, own, p_out, p_in,
    loc_sem, know, hs, hr, ds_, dr, s1, r1, s2, r2, sx, rx,
):
    length, inner = x_ref.shape
    gw = b_ref.shape[1]
    heads = dt_ref.shape[0]
    tiles = inner // LANES
    per_group_tiles = tiles // (gw // STATE)
    stride = n // owners
    rows = tiles * STATE // owners
    taps = tx_ref.shape[0]
    half = length // 2
    chunks, _, cols = p_out.shape
    me = lax.axis_index("sp")
    core = lax.axis_index("tp")
    mate = 1 - core

    barrier = pltpu.get_barrier_semaphore()
    bits = (n - 1).bit_length()
    for bit in range(bits):
        other = me + (1 - 2 * lax.rem(me // (1 << bit), 2)) * (1 << bit)
        pl.semaphore_signal(barrier, inc=1, device_id={"sp": other}, device_id_type=MESH)
    pl.semaphore_signal(barrier, inc=1, device_id={"tp": mate}, device_id_type=MESH)

    @pl.when(me > 0)
    def _():
        pl.semaphore_signal(barrier, inc=1, device_id={"sp": me - 1}, device_id_type=MESH)

    @pl.when(me < n - 1)
    def _():
        pl.semaphore_signal(barrier, inc=1, device_id={"sp": me + 1}, device_id_type=MESH)

    loads = [
        pltpu.make_async_copy(src, dst, loc_sem.at[i])
        for i, (src, dst) in enumerate((
            (x_hbm, x_ref), (b_hbm, b_ref), (c_hbm, c_ref), (dt_hbm, dt_ref),
            (fade_hbm, fade_ref), (off_hbm, off_ref), (speed_hbm, speed_ref),
            (tx_hbm, tx_ref), (tb_hbm, tb_ref), (tc_hbm, tc_ref),
            (gain_hbm, gain_ref), (z_hbm, z_ref), (w_hbm, w_ref),
        ))
    ]
    for load in loads:
        load.start()

    edge = halo_x.shape[0]
    halos = [
        pltpu.make_async_remote_copy(
            src_ref=src.at[pl.ds(length - edge, edge)],
            dst_ref=dst,
            send_sem=hs.at[i],
            recv_sem=hr.at[i],
            device_id={"sp": lax.rem(me + 1, n)},
            device_id_type=MESH,
        )
        for i, (src, dst) in enumerate(((x_ref, halo_x), (b_ref, halo_b), (c_ref, halo_c)))
    ]

    for load in loads[:10]:
        load.wait()

    inside = (me > 0).astype(jnp.int32) + (me < n - 1).astype(jnp.int32)
    pl.semaphore_wait(barrier, bits + 1 + inside)

    @pl.when(me < n - 1)
    def _():
        for copy in halos:
            copy.start()

    def tell(bit):
        other = me + (1 - 2 * lax.rem(me // (1 << bit), 2)) * (1 << bit)
        pl.semaphore_signal(know.at[bit], inc=1, device_id={"sp": other}, device_id_type=MESH)

    def hear(bit):
        pl.semaphore_wait(know.at[bit], 1)

    tell(0)

    sub = lax.broadcasted_iota(jnp.int32, (heads, length), 0)
    off = jnp.zeros((heads, length), F32)
    speed = jnp.zeros((heads, length), F32)
    for h in range(heads):
        off = jnp.where(sub == h, off_ref[h], off)
        speed = jnp.where(sub == h, speed_ref[h], speed)
    v = dt_ref[...].astype(F32) + off
    step_t = jnp.maximum(v, 0.0) + jnp.log1p(jnp.exp(-jnp.abs(v)))
    log_t = fade_ref[...] - step_t * speed
    r_i = lax.broadcasted_iota(jnp.int32, (length, length), 0)
    c_i = lax.broadcasted_iota(jnp.int32, (length, length), 1)
    causal = r_i >= c_i
    lower = causal.astype(F32)
    eye = (r_i == c_i).astype(F32)
    nt = (((1,), (1,)), ((), ()))
    within = lax.dot_general(lower, log_t, nt, precision=EXACT, preferred_element_type=F32)
    step = lax.dot_general(eye, step_t, nt, precision=EXACT, preferred_element_type=F32)
    within_t = lax.dot_general(log_t, lower, nt, precision=EXACT, preferred_element_type=F32)
    spread = (
        lax.broadcasted_iota(jnp.int32, (heads, inner), 0)
        == lax.broadcasted_iota(jnp.int32, (heads, inner), 1) // HEAD_DIM
    ).astype(F32)
    step_e[...] = jnp.dot(step, spread, precision=EXACT, preferred_element_type=F32)
    within_e = jnp.dot(within, spread, precision=EXACT, preferred_element_type=F32)
    last = within_e[length - 1 :]
    end_e[...] = jnp.exp(last - within_e)
    grow_e[...] = jnp.exp(within_e)
    whole = jnp.exp(last)
    for t in range(tiles):
        dec[t] = whole[:, t * LANES : (t + 1) * LANES]

    lead = 8
    joined[:lead] = jnp.zeros((lead, inner + 2 * gw), F32)
    joined[lead:, :inner] = x_ref[...].astype(F32)
    joined[lead:, inner : inner + gw] = b_ref[...].astype(F32)
    joined[lead:, inner + gw :] = c_ref[...].astype(F32)

    def conv(tap_ref, first, width, start, count):
        coef = tap_ref[...].astype(F32)
        total = jnp.zeros((count, width), F32)
        for k in range(taps):
            begin = lead - (taps - 1) + k + start
            total += coef[k : k + 1] * joined[begin : begin + count, first : first + width]
        return silu(total).astype(BF16)

    def mixed(start, count):
        where = slice(start, start + count)
        scaled = conv(tx_ref, 0, inner, start, count).astype(F32) * step_e[where]
        xs[where] = scaled.astype(BF16)
        xe[where] = (scaled * end_e[where]).astype(BF16)
        cb[where] = conv(tb_ref, inner, gw, start, count)
        cc[where] = conv(tc_ref, inner + gw, gw, start, count)

    mixed(0, length)

    for bit in range(bits - 1):
        hear(bit)
        if bit + 1 < bits - 1:
            tell(bit + 1)

    base = me // stride
    tile_of = owners // tiles

    def dec_copy(owner, slot):
        return pltpu.make_async_remote_copy(
            src_ref=dec.at[owner // tile_of],
            dst_ref=dec_in.at[slot],
            send_sem=ds_.at[owner],
            recv_sem=dr.at[slot],
            device_id={"sp": owner * stride},
            device_id_type=MESH,
        )

    def st_copy(owner, slot):
        return pltpu.make_async_remote_copy(
            src_ref=st.at[owner],
            dst_ref=st_in.at[slot],
            send_sem=s1.at[owner],
            recv_sem=r1.at[slot],
            device_id={"sp": owner * stride},
            device_id_type=MESH,
        )

    def ent_copy(place, slot):
        return pltpu.make_async_remote_copy(
            src_ref=eb.at[place],
            dst_ref=ent.at[slot],
            send_sem=s2.at[place],
            recv_sem=r2.at[slot],
            device_id={"sp": place},
            device_id_type=MESH,
        )

    def to_owners(make, method, slot):
        def body(i, carry):
            owner = lax.rem(base + i, owners)

            @pl.when(owner * stride != me)
            def _():
                getattr(make(owner, slot), method)()

            return carry

        lax.fori_loop(0, owners, body, 0)

    is_owner = lax.rem(me, stride) == 0
    to_owners(dec_copy, "start", me)

    @pl.when(is_owner)
    def _():
        dec_in[me] = dec[base // tile_of]

    @pl.when(me > 0)
    def _():
        for copy in halos:
            copy.wait_recv()
        joined[:lead, :inner] = halo_x[...].astype(F32)[edge - lead :]
        joined[:lead, inner : inner + gw] = halo_b[...].astype(F32)[edge - lead :]
        joined[:lead, inner + gw :] = halo_c[...].astype(F32)[edge - lead :]
        mixed(0, 16)

    cb_t = cb[...].astype(F32).T.astype(BF16)
    per_tile = STATE // rows
    for t in range(tiles):
        g = t // per_group_tiles
        s = jnp.dot(
            cb_t[g * STATE : (g + 1) * STATE],
            xe[:, t * LANES : (t + 1) * LANES],
            preferred_element_type=F32,
        )
        for j in range(per_tile):
            st[t * per_tile + j] = s[j * rows : (j + 1) * rows].astype(BF16)

    to_owners(st_copy, "start", me)

    @pl.when(is_owner)
    def _():
        st_in[me] = st[base]

    low_lanes = lax.broadcasted_iota(jnp.int32, (length, LANES), 1) < HEAD_DIM
    for t in range(tiles):
        g = t // per_group_tiles
        if t % per_group_tiles == 0:
            scores = jnp.dot(
                cc[:, g * STATE : (g + 1) * STATE],
                cb_t[g * STATE : (g + 1) * STATE],
                preferred_element_type=F32,
            )
        parts = []
        for h in (2 * t, 2 * t + 1):
            gap = within[:, h : h + 1] - within_t[h : h + 1]
            weight = (scores * jnp.exp(jnp.where(causal, gap, -jnp.inf))).astype(BF16)
            parts.append(
                jnp.dot(
                    weight, xs[:, t * LANES : (t + 1) * LANES], preferred_element_type=F32
                )
            )
        y_in[:, t * LANES : (t + 1) * LANES] = jnp.where(low_lanes, parts[0], parts[1])
    loads[10].wait()
    loads[11].wait()
    gate[...] = silu(z_ref[...].astype(F32))

    @pl.when(is_owner)
    def _():
        def turn(k, state):
            @pl.when(k != me)
            def _():
                dec_copy(base, k).wait_recv()
                st_copy(base, k).wait_recv()

            eb[k] = state.astype(BF16)
            return dec_in[k] * state + st_in[k].astype(F32)

        lax.fori_loop(0, n, turn, jnp.zeros((rows, LANES), F32))

        def deliver(i, carry):
            ent_copy(lax.rem(me + i, n), base).start()
            return carry

        lax.fori_loop(1, n, deliver, 0)
        ent[base] = eb[me]

    def arrive(owner, carry):
        @pl.when(owner * stride != me)
        def _():
            ent_copy(me, owner).wait_recv()

        return carry

    lax.fori_loop(0, owners, arrive, 0)

    gain = gain_ref[...].astype(F32).reshape(1, inner)
    total = jnp.zeros((length, 1), F32)
    for t in range(tiles):
        g = t // per_group_tiles
        lanes = slice(t * LANES, (t + 1) * LANES)
        held = ent[t * per_tile : (t + 1) * per_tile].reshape(STATE, LANES)
        read = jnp.dot(cc[:, g * STATE : (g + 1) * STATE], held, preferred_element_type=F32)
        gated = (y_in[:, lanes] + grow_e[:, lanes] * read) * gate[:, lanes]
        total += jnp.sum(gated * gated, axis=1, keepdims=True)
        gg[:, lanes] = (gated * gain[:, lanes]).astype(BF16)
    ssq[...] = jnp.broadcast_to(total, (length, LANES))

    def mate_copy(src, dst, i):
        return pltpu.make_async_remote_copy(
            src_ref=src,
            dst_ref=dst,
            send_sem=sx.at[i],
            recv_sem=rx.at[i],
            device_id={"tp": mate},
            device_id_type=MESH,
        )

    theirs = pl.ds(pl.multiple_of(mate * half, half), half)
    mine = pl.ds(pl.multiple_of(core * half, half), half)
    first = mate_copy(ssq.at[theirs], ssq_in, chunks)
    first.start()
    loads[12].wait()
    sent = []
    for i in range(chunks):
        own[i] = jnp.dot(
            gg[...], w_ref[:, i * cols : (i + 1) * cols], preferred_element_type=F32
        )
        p_out[i] = own[i, theirs].astype(BF16)
        copy = mate_copy(p_out.at[i], p_in.at[i], i)
        copy.start()
        sent.append(copy)
    first.wait_recv()
    mean = (ssq[mine] + ssq_in[...]) * (1.0 / (2 * inner))
    scale = lax.rsqrt(mean + EPS)[:, :1]
    for i in range(chunks):
        sent[i].wait_recv()
        out_ref[:, i * cols : (i + 1) * cols] = (
            (own[i, mine] + p_in[i].astype(F32)) * scale
        ).astype(BF16)

    @pl.when(me < n - 1)
    def _():
        for copy in halos:
            copy.wait_send()

    to_owners(dec_copy, "wait_send", me)
    to_owners(st_copy, "wait_send", me)

    @pl.when(is_owner)
    def _():
        def sent_one(i, carry):
            ent_copy(lax.rem(me + i, n), base).wait_send()
            return carry

        lax.fori_loop(1, n, sent_one, 0)

    first.wait_send()
    for copy in sent:
        copy.wait_send()


def per_device(n, x, b, c, z, dt, fade, tx, tb, tc, off, speed, gain, w):
    length, inner = x.shape
    gw = b.shape[1]
    width = w.shape[1]
    tiles = inner // LANES
    owners = min(n, tiles * STATE // 16)
    rows = tiles * STATE // owners
    half = length // 2
    chunks = 4
    cols = width // chunks
    vmem = pl.BlockSpec(memory_space=pltpu.VMEM)
    hbm = pl.BlockSpec(memory_space=pl.ANY)
    V = pltpu.VMEM
    dma = lambda k: pltpu.SemaphoreType.DMA((k,))
    return pl.pallas_call(
        functools.partial(kernel, n, owners),
        out_shape=pltpu.VMEM((half, width), BF16),
        in_specs=[hbm] * 13,
        out_specs=vmem,
        scratch_shapes=[
            V(x.shape, BF16),
            V(b.shape, BF16),
            V(c.shape, BF16),
            V(z.shape, BF16),
            V(dt.shape[::-1], BF16),
            V(fade.shape[::-1], F32),
            V(tx.shape, BF16),
            V(tb.shape, BF16),
            V(tc.shape, BF16),
            pltpu.SMEM(off.shape, F32),
            pltpu.SMEM(speed.shape, F32),
            V(gain.shape, BF16),
            V(w.shape, BF16),
            V((16, inner), BF16),
            V((16, gw), BF16),
            V((16, gw), BF16),
            V((length + 8, inner + 2 * gw), F32),
            V((length, inner), BF16),
            V((length, inner), BF16),
            V((length, gw), BF16),
            V((length, gw), BF16),
            V((length, inner), F32),
            V((length, inner), F32),
            V((length, inner), F32),
            V((length, inner), F32),
            V((length, inner), F32),
            V((tiles, 1, LANES), F32),
            V((n, 1, LANES), F32),
            V((owners, rows, LANES), BF16),
            V((n, rows, LANES), BF16),
            V((n, rows, LANES), BF16),
            V((owners, rows, LANES), BF16),
            V((length, inner), BF16),
            V((length, LANES), F32),
            V((half, LANES), F32),
            V((chunks, length, cols), F32),
            V((chunks, half, cols), BF16),
            V((chunks, half, cols), BF16),
            dma(13), pltpu.SemaphoreType.REGULAR((max(1, (n - 1).bit_length()),)), dma(3), dma(3), dma(owners), dma(n), dma(owners), dma(n),
            dma(n), dma(owners), dma(chunks + 1), dma(chunks + 1),
        ],
        compiler_params=pltpu.CompilerParams(collective_id=0, has_side_effects=True),
    )(x, b, c, z, dt.T, fade.T, tx, tb, tc, off, speed, gain, w)


def solution(mesh):
    both = P("sp", "tp")
    taps = P(None, "tp")
    placed = (both,) * 6 + (taps,) * 3 + (P("tp"),) * 3 + (P("tp", None),)
    return jax.shard_map(
        functools.partial(per_device, mesh.shape["sp"]),
        mesh=mesh,
        in_specs=placed,
        out_specs=P(("sp", "tp"), None),
        check_vma=False,
    )
```

```python
import functools

import jax
import jax.numpy as jnp
from jax import lax
from jax.experimental import pallas as pl
from jax.experimental.pallas import tpu as pltpu
from jax.sharding import PartitionSpec as P

HEAD_DIM = 64
STATE = 64
LANES = 128
EPS = 1e-05
EXACT = lax.Precision.HIGHEST
MESH = pl.DeviceIdType.MESH
F32 = jnp.float32
BF16 = jnp.bfloat16


def silu(v):
    return v / (1.0 + jnp.exp(-v))


def kernel(
    n, owners,
    x_hbm, b_hbm, c_hbm, z_hbm, dt_hbm, fade_hbm, tx_hbm, tb_hbm, tc_hbm,
    off_hbm, speed_hbm, gain_hbm, w_hbm,
    out_hbm,
    out_ref, x_ref, b_ref, c_ref, z_ref, dt_ref, fade_ref, tx_ref, tb_ref, tc_ref,
    off_ref, speed_ref, gain_ref, w_ref, halo_x, halo_b, halo_c, joined, xs, xe, cb, cc, step_e, end_e, grow_e,
    gate, y_in, dec, dec_in, st, st_in, eb, ent, gg, ssq, ssq_in, own, p_out, p_in,
    loc_sem, put_sem, know, hs, hr, ds_, dr, s1, r1, s2, r2, sx, rx,
):
    length, inner = x_ref.shape
    gw = b_ref.shape[1]
    heads = dt_ref.shape[0]
    tiles = inner // LANES
    per_group_tiles = tiles // (gw // STATE)
    front = n // 4
    stride = (n // 2) // owners
    rows = tiles * STATE // owners
    taps = tx_ref.shape[0]
    half = length // 2
    chunks, _, cols = p_out.shape
    me = lax.axis_index("sp")
    core = lax.axis_index("tp")
    mate = 1 - core
    shifted = lax.rem(me + n - front, n)

    barrier = pltpu.get_barrier_semaphore()
    bits = (n - 1).bit_length()
    for bit in range(bits):
        other = me + (1 - 2 * lax.rem(me // (1 << bit), 2)) * (1 << bit)
        pl.semaphore_signal(barrier, inc=1, device_id={"sp": other}, device_id_type=MESH)
    pl.semaphore_signal(barrier, inc=1, device_id={"tp": mate}, device_id_type=MESH)

    @pl.when(me > 0)
    def _():
        pl.semaphore_signal(barrier, inc=1, device_id={"sp": me - 1}, device_id_type=MESH)

    @pl.when(me < n - 1)
    def _():
        pl.semaphore_signal(barrier, inc=1, device_id={"sp": me + 1}, device_id_type=MESH)

    loads = [
        pltpu.make_async_copy(src, dst, loc_sem.at[i])
        for i, (src, dst) in enumerate((
            (x_hbm, x_ref), (b_hbm, b_ref), (c_hbm, c_ref), (dt_hbm, dt_ref),
            (fade_hbm, fade_ref), (off_hbm, off_ref), (speed_hbm, speed_ref),
            (tx_hbm, tx_ref), (tb_hbm, tb_ref), (tc_hbm, tc_ref),
            (gain_hbm, gain_ref), (z_hbm, z_ref), (w_hbm, w_ref),
        ))
    ]
    for load in loads:
        load.start()

    edge = halo_x.shape[0]
    halos = [
        pltpu.make_async_remote_copy(
            src_ref=src.at[pl.ds(length - edge, edge)],
            dst_ref=dst,
            send_sem=hs.at[i],
            recv_sem=hr.at[i],
            device_id={"sp": lax.rem(me + 1, n)},
            device_id_type=MESH,
        )
        for i, (src, dst) in enumerate(((x_ref, halo_x), (b_ref, halo_b), (c_ref, halo_c)))
    ]

    for load in loads[:10]:
        load.wait()

    inside = (me > 0).astype(jnp.int32) + (me < n - 1).astype(jnp.int32)
    pl.semaphore_wait(barrier, bits + 1 + inside)

    @pl.when(me < n - 1)
    def _():
        for copy in halos:
            copy.start()

    def tell(bit):
        other = me + (1 - 2 * lax.rem(me // (1 << bit), 2)) * (1 << bit)
        pl.semaphore_signal(know.at[bit], inc=1, device_id={"sp": other}, device_id_type=MESH)

    def hear(bit):
        pl.semaphore_wait(know.at[bit], 1)

    tell(0)

    sub = lax.broadcasted_iota(jnp.int32, (heads, length), 0)
    off = jnp.zeros((heads, length), F32)
    speed = jnp.zeros((heads, length), F32)
    for h in range(heads):
        off = jnp.where(sub == h, off_ref[h], off)
        speed = jnp.where(sub == h, speed_ref[h], speed)
    v = dt_ref[...].astype(F32) + off
    step_t = jnp.maximum(v, 0.0) + jnp.log1p(jnp.exp(-jnp.abs(v)))
    log_t = fade_ref[...] - step_t * speed
    r_i = lax.broadcasted_iota(jnp.int32, (length, length), 0)
    c_i = lax.broadcasted_iota(jnp.int32, (length, length), 1)
    causal = r_i >= c_i
    lower = causal.astype(F32)
    eye = (r_i == c_i).astype(F32)
    nt = (((1,), (1,)), ((), ()))
    within = lax.dot_general(lower, log_t, nt, precision=EXACT, preferred_element_type=F32)
    step = lax.dot_general(eye, step_t, nt, precision=EXACT, preferred_element_type=F32)
    within_t = lax.dot_general(log_t, lower, nt, precision=EXACT, preferred_element_type=F32)
    spread = (
        lax.broadcasted_iota(jnp.int32, (heads, inner), 0)
        == lax.broadcasted_iota(jnp.int32, (heads, inner), 1) // HEAD_DIM
    ).astype(F32)
    step_e[...] = jnp.dot(step, spread, precision=EXACT, preferred_element_type=F32)
    within_e = jnp.dot(within, spread, precision=EXACT, preferred_element_type=F32)
    last = within_e[length - 1 :]
    end_e[...] = jnp.exp(last - within_e)
    grow_e[...] = jnp.exp(within_e)
    whole = jnp.exp(last)
    for t in range(tiles):
        dec[t] = whole[:, t * LANES : (t + 1) * LANES]

    lead = 8
    joined[:lead] = jnp.zeros((lead, inner + 2 * gw), F32)
    joined[lead:, :inner] = x_ref[...].astype(F32)
    joined[lead:, inner : inner + gw] = b_ref[...].astype(F32)
    joined[lead:, inner + gw :] = c_ref[...].astype(F32)

    def conv(tap_ref, first, width, start, count):
        coef = tap_ref[...].astype(F32)
        total = jnp.zeros((count, width), F32)
        for k in range(taps):
            begin = lead - (taps - 1) + k + start
            total += coef[k : k + 1] * joined[begin : begin + count, first : first + width]
        return silu(total).astype(BF16)

    def mixed(start, count):
        where = slice(start, start + count)
        scaled = conv(tx_ref, 0, inner, start, count).astype(F32) * step_e[where]
        xs[where] = scaled.astype(BF16)
        xe[where] = (scaled * end_e[where]).astype(BF16)
        cb[where] = conv(tb_ref, inner, gw, start, count)
        cc[where] = conv(tc_ref, inner + gw, gw, start, count)

    mixed(0, length)

    for bit in range(bits - 2):
        hear(bit)
        tell(bit + 1)
    middle = shifted < n // 2

    @pl.when(middle)
    def _():
        hear(bits - 2)

    base = lax.rem(shifted // stride, owners)
    tile_of = owners // tiles

    def dec_copy(owner, slot):
        return pltpu.make_async_remote_copy(
            src_ref=dec.at[owner // tile_of],
            dst_ref=dec_in.at[slot],
            send_sem=ds_.at[owner],
            recv_sem=dr.at[slot],
            device_id={"sp": front + owner * stride},
            device_id_type=MESH,
        )

    def st_copy(owner, slot):
        return pltpu.make_async_remote_copy(
            src_ref=st.at[owner],
            dst_ref=st_in.at[slot],
            send_sem=s1.at[owner],
            recv_sem=r1.at[slot],
            device_id={"sp": front + owner * stride},
            device_id_type=MESH,
        )

    def ent_copy(place, slot):
        return pltpu.make_async_remote_copy(
            src_ref=eb.at[place],
            dst_ref=ent.at[slot],
            send_sem=s2.at[place],
            recv_sem=r2.at[slot],
            device_id={"sp": place},
            device_id_type=MESH,
        )

    def to_owners(make, method, slot):
        def body(i, carry):
            owner = lax.rem(base + i, owners)

            @pl.when(front + owner * stride != me)
            def _():
                getattr(make(owner, slot), method)()

            return carry

        lax.fori_loop(0, owners, body, 0)

    is_owner = (shifted < n // 2) & (lax.rem(shifted, stride) == 0)
    to_owners(dec_copy, "start", me)

    @pl.when(is_owner)
    def _():
        dec_in[me] = dec[base // tile_of]

    @pl.when(me > 0)
    def _():
        for copy in halos:
            copy.wait_recv()
        joined[:lead, :inner] = halo_x[...].astype(F32)[edge - lead :]
        joined[:lead, inner : inner + gw] = halo_b[...].astype(F32)[edge - lead :]
        joined[:lead, inner + gw :] = halo_c[...].astype(F32)[edge - lead :]
        mixed(0, 16)

    cb_t = cb[...].astype(F32).T.astype(BF16)
    per_tile = STATE // rows
    for t in range(tiles):
        g = t // per_group_tiles
        s = jnp.dot(
            cb_t[g * STATE : (g + 1) * STATE],
            xe[:, t * LANES : (t + 1) * LANES],
            preferred_element_type=F32,
        )
        for j in range(per_tile):
            st[t * per_tile + j] = s[j * rows : (j + 1) * rows].astype(BF16)

    to_owners(st_copy, "start", me)

    @pl.when(is_owner)
    def _():
        st_in[me] = st[base]

    low_lanes = lax.broadcasted_iota(jnp.int32, (length, LANES), 1) < HEAD_DIM
    for t in range(tiles):
        g = t // per_group_tiles
        if t % per_group_tiles == 0:
            scores = jnp.dot(
                cc[:, g * STATE : (g + 1) * STATE],
                cb_t[g * STATE : (g + 1) * STATE],
                preferred_element_type=F32,
            )
        parts = []
        for h in (2 * t, 2 * t + 1):
            gap = within[:, h : h + 1] - within_t[h : h + 1]
            weight = (scores * jnp.exp(jnp.where(causal, gap, -jnp.inf))).astype(BF16)
            parts.append(
                jnp.dot(
                    weight, xs[:, t * LANES : (t + 1) * LANES], preferred_element_type=F32
                )
            )
        y_in[:, t * LANES : (t + 1) * LANES] = jnp.where(low_lanes, parts[0], parts[1])
    loads[10].wait()
    loads[11].wait()
    gate[...] = silu(z_ref[...].astype(F32))

    @pl.when(is_owner)
    def _():
        def turn(k, state):
            @pl.when(k != me)
            def _():
                dec_copy(base, k).wait_recv()
                st_copy(base, k).wait_recv()

            eb[k] = state.astype(BF16)
            return dec_in[k] * state + st_in[k].astype(F32)

        lax.fori_loop(0, n, turn, jnp.zeros((rows, LANES), F32))

        def deliver(i, carry):
            place = lax.rem(me + i, n)

            @pl.when(place > 0)
            def _():
                ent_copy(place, base).start()

            return carry

        lax.fori_loop(1, n, deliver, 0)
        ent[base] = eb[me]

    @pl.when(jnp.logical_not(middle))
    def _():
        hear(bits - 2)

    @pl.when(me == 0)
    def _():
        ent[...] = jnp.zeros_like(ent)

    def arrive(owner, carry):
        @pl.when(front + owner * stride != me)
        def _():
            ent_copy(me, owner).wait_recv()

        return carry

    @pl.when(me > 0)
    def _():
        lax.fori_loop(0, owners, arrive, 0)

    gain = gain_ref[...].astype(F32).reshape(1, inner)
    total = jnp.zeros((length, 1), F32)
    for t in range(tiles):
        g = t // per_group_tiles
        lanes = slice(t * LANES, (t + 1) * LANES)
        held = ent[t * per_tile : (t + 1) * per_tile].reshape(STATE, LANES)
        read = jnp.dot(cc[:, g * STATE : (g + 1) * STATE], held, preferred_element_type=F32)
        gated = (y_in[:, lanes] + grow_e[:, lanes] * read) * gate[:, lanes]
        total += jnp.sum(gated * gated, axis=1, keepdims=True)
        gg[:, lanes] = (gated * gain[:, lanes]).astype(BF16)
    ssq[...] = jnp.broadcast_to(total, (length, LANES))

    def mate_copy(src, dst, i):
        return pltpu.make_async_remote_copy(
            src_ref=src,
            dst_ref=dst,
            send_sem=sx.at[i],
            recv_sem=rx.at[i],
            device_id={"tp": mate},
            device_id_type=MESH,
        )

    theirs = pl.ds(pl.multiple_of(mate * half, half), half)
    mine = pl.ds(pl.multiple_of(core * half, half), half)
    first = mate_copy(ssq.at[theirs], ssq_in, chunks)
    first.start()
    loads[12].wait()
    sent = []
    for i in range(chunks):
        own[i] = jnp.dot(
            gg[...], w_ref[:, i * cols : (i + 1) * cols], preferred_element_type=F32
        )
        p_out[i] = own[i, theirs].astype(BF16)
        copy = mate_copy(p_out.at[i], p_in.at[i], i)
        copy.start()
        sent.append(copy)
    first.wait_recv()
    mean = (ssq[mine] + ssq_in[...]) * (1.0 / (2 * inner))
    scale = lax.rsqrt(mean + EPS)[:, :1]
    puts = []
    for i in range(chunks):
        sent[i].wait_recv()
        out_ref[:, i * cols : (i + 1) * cols] = (
            (own[i, mine] + p_in[i].astype(F32)) * scale
        ).astype(BF16)
        put = pltpu.make_async_copy(
            out_ref.at[:, i * cols : (i + 1) * cols],
            out_hbm.at[:, i * cols : (i + 1) * cols],
            put_sem.at[i],
        )
        put.start()
        puts.append(put)

    @pl.when(me < n - 1)
    def _():
        for copy in halos:
            copy.wait_send()

    to_owners(dec_copy, "wait_send", me)
    to_owners(st_copy, "wait_send", me)

    @pl.when(is_owner)
    def _():
        def sent_one(i, carry):
            place = lax.rem(me + i, n)

            @pl.when(place > 0)
            def _():
                ent_copy(place, base).wait_send()

            return carry

        lax.fori_loop(1, n, sent_one, 0)

    first.wait_send()
    for copy in sent:
        copy.wait_send()
    for put in puts:
        put.wait()


def per_device(n, x, b, c, z, dt, fade, tx, tb, tc, off, speed, gain, w):
    length, inner = x.shape
    gw = b.shape[1]
    width = w.shape[1]
    tiles = inner // LANES
    owners = min(n // 2, tiles * STATE // 16)
    rows = tiles * STATE // owners
    half = length // 2
    chunks = 4
    cols = width // chunks
    vmem = pl.BlockSpec(memory_space=pltpu.VMEM)
    hbm = pl.BlockSpec(memory_space=pl.ANY)
    V = pltpu.VMEM
    dma = lambda k: pltpu.SemaphoreType.DMA((k,))
    return pl.pallas_call(
        functools.partial(kernel, n, owners),
        out_shape=pltpu.VMEM((half, width), BF16),
        in_specs=[hbm] * 13,
        out_specs=hbm,
        scratch_shapes=[
            V((half, width), BF16),
            V(x.shape, BF16),
            V(b.shape, BF16),
            V(c.shape, BF16),
            V(z.shape, BF16),
            V(dt.shape[::-1], BF16),
            V(fade.shape[::-1], F32),
            V(tx.shape, BF16),
            V(tb.shape, BF16),
            V(tc.shape, BF16),
            pltpu.SMEM(off.shape, F32),
            pltpu.SMEM(speed.shape, F32),
            V(gain.shape, BF16),
            V(w.shape, BF16),
            V((16, inner), BF16),
            V((16, gw), BF16),
            V((16, gw), BF16),
            V((length + 8, inner + 2 * gw), F32),
            V((length, inner), BF16),
            V((length, inner), BF16),
            V((length, gw), BF16),
            V((length, gw), BF16),
            V((length, inner), F32),
            V((length, inner), F32),
            V((length, inner), F32),
            V((length, inner), F32),
            V((length, inner), F32),
            V((tiles, 1, LANES), F32),
            V((n, 1, LANES), F32),
            V((owners, rows, LANES), BF16),
            V((n, rows, LANES), BF16),
            V((n, rows, LANES), BF16),
            V((owners, rows, LANES), BF16),
            V((length, inner), BF16),
            V((length, LANES), F32),
            V((half, LANES), F32),
            V((chunks, length, cols), F32),
            V((chunks, half, cols), BF16),
            V((chunks, half, cols), BF16),
            dma(13), dma(chunks), pltpu.SemaphoreType.REGULAR((max(1, (n - 1).bit_length()),)), dma(3), dma(3), dma(owners), dma(n), dma(owners), dma(n),
            dma(n), dma(owners), dma(chunks + 1), dma(chunks + 1),
        ],
        compiler_params=pltpu.CompilerParams(collective_id=0, has_side_effects=True),
    )(x, b, c, z, dt.T, fade.T, tx, tb, tc, off, speed, gain, w)


def solution(mesh):
    both = P("sp", "tp")
    taps = P(None, "tp")
    placed = (both,) * 6 + (taps,) * 3 + (P("tp"),) * 3 + (P("tp", None),)
    return jax.shard_map(
        functools.partial(per_device, mesh.shape["sp"]),
        mesh=mesh,
        in_specs=placed,
        out_specs=P(("sp", "tp"), None),
        check_vma=False,
    )
```

```python
import functools

import jax
import jax.numpy as jnp
from jax import lax
from jax.experimental import pallas as pl
from jax.experimental.pallas import tpu as pltpu
from jax.sharding import PartitionSpec as P

HEAD_DIM = 64
STATE = 64
LANES = 128
EPS = 1e-05
EXACT = lax.Precision.HIGHEST
MESH = pl.DeviceIdType.MESH
F32 = jnp.float32
BF16 = jnp.bfloat16


def silu(v):
    return v / (1.0 + jnp.exp(-v))


def kernel(
    n, owners,
    x_hbm, b_hbm, c_hbm, z_hbm, dt_hbm, fade_hbm, tx_hbm, tb_hbm, tc_hbm,
    off_hbm, speed_hbm, gain_hbm, w_hbm,
    out_hbm,
    out_ref, x_ref, b_ref, c_ref, z_ref, dt_ref, fade_ref, tx_ref, tb_ref, tc_ref,
    off_ref, speed_ref, gain_ref, w_ref, halo_x, halo_b, halo_c, joined, xs, xe, cb, cc, step_e, end_e, grow_e,
    gate, y_in, dec, dec_in, st, st_in, eb, ent, gg, ssq, ssq_in, own, p_out, p_in,
    loc_sem, put_sem, know, hs, hr, ds_, dr, s1, r1, s2, r2, sx, rx,
):
    length, inner = x_ref.shape
    gw = b_ref.shape[1]
    heads = dt_ref.shape[0]
    tiles = inner // LANES
    per_group_tiles = tiles // (gw // STATE)
    front = n // 4
    stride = (n // 2) // owners
    rows = tiles * STATE // owners
    taps = tx_ref.shape[0]
    half = length // 2
    chunks, _, cols = p_out.shape
    me = lax.axis_index("sp")
    core = lax.axis_index("tp")
    mate = 1 - core
    shifted = lax.rem(me + n - front, n)

    barrier = pltpu.get_barrier_semaphore()
    bits = (n - 1).bit_length()
    for bit in range(bits):
        other = me + (1 - 2 * lax.rem(me // (1 << bit), 2)) * (1 << bit)
        pl.semaphore_signal(barrier, inc=1, device_id={"sp": other}, device_id_type=MESH)
    pl.semaphore_signal(barrier, inc=1, device_id={"tp": mate}, device_id_type=MESH)

    @pl.when(me > 0)
    def _():
        pl.semaphore_signal(barrier, inc=1, device_id={"sp": me - 1}, device_id_type=MESH)

    @pl.when(me < n - 1)
    def _():
        pl.semaphore_signal(barrier, inc=1, device_id={"sp": me + 1}, device_id_type=MESH)

    loads = [
        pltpu.make_async_copy(src, dst, loc_sem.at[i])
        for i, (src, dst) in enumerate((
            (x_hbm, x_ref), (b_hbm, b_ref), (c_hbm, c_ref), (dt_hbm, dt_ref),
            (fade_hbm, fade_ref), (off_hbm, off_ref), (speed_hbm, speed_ref),
            (tx_hbm, tx_ref), (tb_hbm, tb_ref), (tc_hbm, tc_ref),
            (gain_hbm, gain_ref), (z_hbm, z_ref), (w_hbm, w_ref),
        ))
    ]
    for load in loads:
        load.start()

    edge = halo_x.shape[0]
    halos = [
        pltpu.make_async_remote_copy(
            src_ref=src.at[pl.ds(length - edge, edge)],
            dst_ref=dst,
            send_sem=hs.at[i],
            recv_sem=hr.at[i],
            device_id={"sp": lax.rem(me + 1, n)},
            device_id_type=MESH,
        )
        for i, (src, dst) in enumerate(((x_ref, halo_x), (b_ref, halo_b), (c_ref, halo_c)))
    ]

    for load in loads[:10]:
        load.wait()

    inside = (me > 0).astype(jnp.int32) + (me < n - 1).astype(jnp.int32)
    pl.semaphore_wait(barrier, bits + 1 + inside)

    @pl.when(me < n - 1)
    def _():
        for copy in halos:
            copy.start()

    def tell(bit):
        other = me + (1 - 2 * lax.rem(me // (1 << bit), 2)) * (1 << bit)
        pl.semaphore_signal(know.at[bit], inc=1, device_id={"sp": other}, device_id_type=MESH)

    def hear(bit):
        pl.semaphore_wait(know.at[bit], 1)

    tell(0)

    sub = lax.broadcasted_iota(jnp.int32, (heads, length), 0)
    off = jnp.zeros((heads, length), F32)
    speed = jnp.zeros((heads, length), F32)
    for h in range(heads):
        off = jnp.where(sub == h, off_ref[h], off)
        speed = jnp.where(sub == h, speed_ref[h], speed)
    v = dt_ref[...].astype(F32) + off
    step_t = jnp.maximum(v, 0.0) + jnp.log1p(jnp.exp(-jnp.abs(v)))
    log_t = fade_ref[...] - step_t * speed
    r_i = lax.broadcasted_iota(jnp.int32, (length, length), 0)
    c_i = lax.broadcasted_iota(jnp.int32, (length, length), 1)
    causal = r_i >= c_i
    lower = causal.astype(F32)
    eye = (r_i == c_i).astype(F32)
    nt = (((1,), (1,)), ((), ()))
    within = lax.dot_general(lower, log_t, nt, precision=EXACT, preferred_element_type=F32)
    step = lax.dot_general(eye, step_t, nt, precision=EXACT, preferred_element_type=F32)
    within_t = lax.dot_general(log_t, lower, nt, precision=EXACT, preferred_element_type=F32)
    spread = (
        lax.broadcasted_iota(jnp.int32, (heads, inner), 0)
        == lax.broadcasted_iota(jnp.int32, (heads, inner), 1) // HEAD_DIM
    ).astype(F32)
    step_e[...] = jnp.dot(step, spread, precision=EXACT, preferred_element_type=F32)
    within_e = jnp.dot(within, spread, precision=EXACT, preferred_element_type=F32)
    last = within_e[length - 1 :]
    end_e[...] = jnp.exp(last - within_e)
    grow_e[...] = jnp.exp(within_e)
    whole = jnp.exp(last)
    for t in range(tiles):
        dec[t] = whole[:, t * LANES : (t + 1) * LANES]

    lead = 8
    joined[:lead] = jnp.zeros((lead, inner + 2 * gw), F32)
    joined[lead:, :inner] = x_ref[...].astype(F32)
    joined[lead:, inner : inner + gw] = b_ref[...].astype(F32)
    joined[lead:, inner + gw :] = c_ref[...].astype(F32)

    def conv(tap_ref, first, width, start, count):
        coef = tap_ref[...].astype(F32)
        total = jnp.zeros((count, width), F32)
        for k in range(taps):
            begin = lead - (taps - 1) + k + start
            total += coef[k : k + 1] * joined[begin : begin + count, first : first + width]
        return silu(total).astype(BF16)

    def mixed(start, count):
        where = slice(start, start + count)
        scaled = conv(tx_ref, 0, inner, start, count).astype(F32) * step_e[where]
        xs[where] = scaled.astype(BF16)
        xe[where] = (scaled * end_e[where]).astype(BF16)
        cb[where] = conv(tb_ref, inner, gw, start, count)
        cc[where] = conv(tc_ref, inner + gw, gw, start, count)

    mixed(0, length)

    for bit in range(bits - 2):
        hear(bit)
        tell(bit + 1)
    middle = shifted < n // 2

    @pl.when(middle)
    def _():
        hear(bits - 2)

    base = lax.rem(shifted // stride, owners)
    tile_of = owners // tiles

    def dec_copy(owner, slot):
        return pltpu.make_async_remote_copy(
            src_ref=dec.at[owner // tile_of],
            dst_ref=dec_in.at[slot],
            send_sem=ds_.at[0],
            recv_sem=dr.at[0],
            device_id={"sp": front + owner * stride},
            device_id_type=MESH,
        )

    def st_copy(owner, slot):
        return pltpu.make_async_remote_copy(
            src_ref=st.at[owner],
            dst_ref=st_in.at[slot],
            send_sem=s1.at[0],
            recv_sem=r1.at[0],
            device_id={"sp": front + owner * stride},
            device_id_type=MESH,
        )

    def ent_copy(place, slot):
        return pltpu.make_async_remote_copy(
            src_ref=eb.at[place],
            dst_ref=ent.at[slot],
            send_sem=s2.at[0],
            recv_sem=r2.at[0],
            device_id={"sp": place},
            device_id_type=MESH,
        )

    def drained(ref, count, sem, method):
        part = ref.at[pl.ds(0, count)]
        getattr(pltpu.make_async_remote_copy(
            src_ref=part,
            dst_ref=part,
            send_sem=sem.at[0],
            recv_sem=sem.at[0],
            device_id={"tp": mate},
            device_id_type=MESH,
        ), method)()

    def to_owners(make, method, slot):
        def body(i, carry):
            owner = lax.rem(base + i, owners)

            @pl.when(front + owner * stride != me)
            def _():
                getattr(make(owner, slot), method)()

            return carry

        lax.fori_loop(0, owners, body, 0)

    is_owner = (shifted < n // 2) & (lax.rem(shifted, stride) == 0)
    to_owners(dec_copy, "start", me)

    @pl.when(is_owner)
    def _():
        dec_in[me] = dec[base // tile_of]

    @pl.when(me > 0)
    def _():
        for copy in halos:
            copy.wait_recv()
        joined[:lead, :inner] = halo_x[...].astype(F32)[edge - lead :]
        joined[:lead, inner : inner + gw] = halo_b[...].astype(F32)[edge - lead :]
        joined[:lead, inner + gw :] = halo_c[...].astype(F32)[edge - lead :]
        mixed(0, 16)

    cb_t = cb[...].astype(F32).T.astype(BF16)
    per_tile = STATE // rows
    for t in range(tiles):
        g = t // per_group_tiles
        s = jnp.dot(
            cb_t[g * STATE : (g + 1) * STATE],
            xe[:, t * LANES : (t + 1) * LANES],
            preferred_element_type=F32,
        )
        for j in range(per_tile):
            st[t * per_tile + j] = s[j * rows : (j + 1) * rows].astype(BF16)

    to_owners(st_copy, "start", me)

    @pl.when(is_owner)
    def _():
        st_in[me] = st[base]

    low_lanes = lax.broadcasted_iota(jnp.int32, (length, LANES), 1) < HEAD_DIM
    for t in range(tiles):
        g = t // per_group_tiles
        if t % per_group_tiles == 0:
            scores = jnp.dot(
                cc[:, g * STATE : (g + 1) * STATE],
                cb_t[g * STATE : (g + 1) * STATE],
                preferred_element_type=F32,
            )
        parts = []
        for h in (2 * t, 2 * t + 1):
            gap = within[:, h : h + 1] - within_t[h : h + 1]
            weight = (scores * jnp.exp(jnp.where(causal, gap, -jnp.inf))).astype(BF16)
            parts.append(
                jnp.dot(
                    weight, xs[:, t * LANES : (t + 1) * LANES], preferred_element_type=F32
                )
            )
        y_in[:, t * LANES : (t + 1) * LANES] = jnp.where(low_lanes, parts[0], parts[1])
    loads[10].wait()
    loads[11].wait()
    gate[...] = silu(z_ref[...].astype(F32))

    @pl.when(is_owner)
    def _():
        drained(dec_in, n - 1, dr, "wait_recv")
        drained(st_in, n - 1, r1, "wait_recv")

        def turn(k, state):
            eb[k] = state.astype(BF16)
            return dec_in[k] * state + st_in[k].astype(F32)

        lax.fori_loop(0, n, turn, jnp.zeros((rows, LANES), F32))

        def deliver(i, carry):
            place = lax.rem(me + i, n)

            @pl.when(place > 0)
            def _():
                ent_copy(place, base).start()

            return carry

        lax.fori_loop(1, n, deliver, 0)
        ent[base] = eb[me]

    @pl.when(jnp.logical_not(middle))
    def _():
        hear(bits - 2)

    @pl.when(me == 0)
    def _():
        ent[...] = jnp.zeros_like(ent)

    @pl.when((me > 0) & jnp.logical_not(is_owner))
    def _():
        drained(ent, owners, r2, "wait_recv")

    @pl.when(is_owner)
    def _():
        drained(ent, owners - 1, r2, "wait_recv")

    gain = gain_ref[...].astype(F32).reshape(1, inner)
    total = jnp.zeros((length, 1), F32)
    for t in range(tiles):
        g = t // per_group_tiles
        lanes = slice(t * LANES, (t + 1) * LANES)
        held = ent[t * per_tile : (t + 1) * per_tile].reshape(STATE, LANES)
        read = jnp.dot(cc[:, g * STATE : (g + 1) * STATE], held, preferred_element_type=F32)
        gated = (y_in[:, lanes] + grow_e[:, lanes] * read) * gate[:, lanes]
        total += jnp.sum(gated * gated, axis=1, keepdims=True)
        gg[:, lanes] = (gated * gain[:, lanes]).astype(BF16)
    ssq[...] = jnp.broadcast_to(total, (length, LANES))

    def mate_copy(src, dst, i):
        return pltpu.make_async_remote_copy(
            src_ref=src,
            dst_ref=dst,
            send_sem=sx.at[i],
            recv_sem=rx.at[i],
            device_id={"tp": mate},
            device_id_type=MESH,
        )

    theirs = pl.ds(pl.multiple_of(mate * half, half), half)
    mine = pl.ds(pl.multiple_of(core * half, half), half)
    first = mate_copy(ssq.at[theirs], ssq_in, chunks)
    first.start()
    loads[12].wait()
    sent = []
    for i in range(chunks):
        own[i] = jnp.dot(
            gg[...], w_ref[:, i * cols : (i + 1) * cols], preferred_element_type=F32
        )
        p_out[i] = own[i, theirs].astype(BF16)
        copy = mate_copy(p_out.at[i], p_in.at[i], i)
        copy.start()
        sent.append(copy)
    first.wait_recv()
    mean = (ssq[mine] + ssq_in[...]) * (1.0 / (2 * inner))
    scale = lax.rsqrt(mean + EPS)[:, :1]
    puts = []
    for i in range(chunks):
        sent[i].wait_recv()
        out_ref[:, i * cols : (i + 1) * cols] = (
            (own[i, mine] + p_in[i].astype(F32)) * scale
        ).astype(BF16)
        put = pltpu.make_async_copy(
            out_ref.at[:, i * cols : (i + 1) * cols],
            out_hbm.at[:, i * cols : (i + 1) * cols],
            put_sem.at[i],
        )
        put.start()
        puts.append(put)

    @pl.when(me < n - 1)
    def _():
        for copy in halos:
            copy.wait_send()

    @pl.when(jnp.logical_not(is_owner))
    def _():
        drained(dec_in, owners, ds_, "wait_send")
        drained(st, owners, s1, "wait_send")

    @pl.when(is_owner)
    def _():
        drained(dec_in, owners - 1, ds_, "wait_send")
        drained(st, owners - 1, s1, "wait_send")
        drained(eb, n - 2, s2, "wait_send")

    first.wait_send()
    for copy in sent:
        copy.wait_send()
    for put in puts:
        put.wait()


def per_device(n, x, b, c, z, dt, fade, tx, tb, tc, off, speed, gain, w):
    length, inner = x.shape
    gw = b.shape[1]
    width = w.shape[1]
    tiles = inner // LANES
    owners = min(n // 2, tiles * STATE // 16)
    rows = tiles * STATE // owners
    half = length // 2
    chunks = 4
    cols = width // chunks
    vmem = pl.BlockSpec(memory_space=pltpu.VMEM)
    hbm = pl.BlockSpec(memory_space=pl.ANY)
    V = pltpu.VMEM
    dma = lambda k: pltpu.SemaphoreType.DMA((k,))
    return pl.pallas_call(
        functools.partial(kernel, n, owners),
        out_shape=pltpu.VMEM((half, width), BF16),
        in_specs=[hbm] * 13,
        out_specs=hbm,
        scratch_shapes=[
            V((half, width), BF16),
            V(x.shape, BF16),
            V(b.shape, BF16),
            V(c.shape, BF16),
            V(z.shape, BF16),
            V(dt.shape[::-1], BF16),
            V(fade.shape[::-1], F32),
            V(tx.shape, BF16),
            V(tb.shape, BF16),
            V(tc.shape, BF16),
            pltpu.SMEM(off.shape, F32),
            pltpu.SMEM(speed.shape, F32),
            V(gain.shape, BF16),
            V(w.shape, BF16),
            V((16, inner), BF16),
            V((16, gw), BF16),
            V((16, gw), BF16),
            V((length + 8, inner + 2 * gw), F32),
            V((length, inner), BF16),
            V((length, inner), BF16),
            V((length, gw), BF16),
            V((length, gw), BF16),
            V((length, inner), F32),
            V((length, inner), F32),
            V((length, inner), F32),
            V((length, inner), F32),
            V((length, inner), F32),
            V((tiles, 1, LANES), F32),
            V((n, 1, LANES), F32),
            V((owners, rows, LANES), BF16),
            V((n, rows, LANES), BF16),
            V((n, rows, LANES), BF16),
            V((owners, rows, LANES), BF16),
            V((length, inner), BF16),
            V((length, LANES), F32),
            V((half, LANES), F32),
            V((chunks, length, cols), F32),
            V((chunks, half, cols), BF16),
            V((chunks, half, cols), BF16),
            dma(13), dma(chunks), pltpu.SemaphoreType.REGULAR((max(1, (n - 1).bit_length()),)), dma(3), dma(3), dma(1), dma(1), dma(1), dma(1),
            dma(1), dma(1), dma(chunks + 1), dma(chunks + 1),
        ],
        compiler_params=pltpu.CompilerParams(collective_id=0, has_side_effects=True),
    )(x, b, c, z, dt.T, fade.T, tx, tb, tc, off, speed, gain, w)


def solution(mesh):
    both = P("sp", "tp")
    taps = P(None, "tp")
    placed = (both,) * 6 + (taps,) * 3 + (P("tp"),) * 3 + (P("tp", None),)
    return jax.shard_map(
        functools.partial(per_device, mesh.shape["sp"]),
        mesh=mesh,
        in_specs=placed,
        out_specs=P(("sp", "tp"), None),
        check_vma=False,
    )
```
